32 devices in a mesh: fs: 16 (over z, y, x), tp: 2 (over core).
Axes of the slice: x: 2, y: 2, z: 4, core: 2. Of those that a mesh axis runs over, the one named last changes fastest.
Arguments:
- x_late: bfloat16 [4096, 2048], P('fs'), may hold values from -6 to 6
- x_early: bfloat16 [4096, 2048], P('fs'), may hold values from -6 to 6
- cotangent: bfloat16 [4096, 2048], P('fs'), may hold values from -6 to 6
- w_gate: bfloat16 [2048, 4096], P('fs', 'tp'), may hold values from -0.125 to 0.125
- w_up: bfloat16 [2048, 4096], P('fs', 'tp'), may hold values from -0.125 to 0.125
- w_down: bfloat16 [4096, 2048], P('tp', 'fs'), may hold values from -0.09375 to 0.09375
- conv_taps: float32 [3, 4096], replicated, may hold values from -3 to 3
- conv_bias: float32 [4096], replicated, may hold values from -3 to 3
- grad_down: float32 [4096, 2048], P('tp', 'fs'), may hold values from -60 to 60
Outputs:
- y_late: bfloat16 [4096, 2048], P('fs')
- dx_early: bfloat16 [4096, 2048], P('fs')
- grad_down_out: float32 [4096, 2048], P('tp', 'fs')
The draws below stay inside these ranges and needn't reach their ends.
All inputs are finite; a program needn't handle non-finite values.
Results may differ from the reference program's by a relative error of at most 0.017.
Values may be sent and summed in bfloat16 or wider, within the bound.
A program may use at most 128 MiB of HBM per device.

```python
import jax
import jax.numpy as jnp
from jax import lax

D = 2048
FF = 4096
TAPS = 3
TOK_DEV = 256
TOKENS = 4096
N_FS = 16
N_TP = 2


def strengthened(array, stream_key, source, target, blocks, factor):
    owner, partner = [(jnp.arange(array.shape[dim]) // (array.shape[dim] // blocks)).reshape([-1 if axis == dim else 1 for axis in range(array.ndim)]) for dim in (source, target)]
    chosen = jax.random.permutation(stream_key, blocks)[partner]
    strong = (owner == chosen) | (owner == (partner + blocks // 2) % blocks)
    return jnp.where(strong, factor * array, array)


def shard_levels(rng, dims, shards, smallest, top_value):
    level, own = 1.0, jax.random.fold_in(rng, 6)
    for axis_at, parts in shards:
        steps = jnp.exp(jax.random.uniform(jax.random.fold_in(own, axis_at), (parts,), jnp.float32, smallest / len(shards), top_value / len(shards)))
        level = level * jnp.repeat(steps, dims[axis_at] // parts).reshape([-1 if axis == axis_at else 1 for axis in range(len(dims))])
    return level


def scatter_about(rng, dims, spread, bound, cuts=(), dtype=jnp.bfloat16):
    loudness = shard_levels(rng, dims, cuts, -0.22, 0.18) if cuts else 1.0
    array = jax.random.normal(rng, dims, jnp.float32) * spread * loudness
    return jnp.minimum(jnp.maximum(array, -bound), bound).astype(dtype)


def bell_draw_with(key, dims, scale, bound, split, heavy, held_as=jnp.bfloat16):
    values = scale * jax.random.normal(key, dims, jnp.float32)
    if split:
        values = values * shard_levels(key, dims, split, -0.22, 0.18)
    return jnp.clip(strengthened(values, jax.random.fold_in(key, 3), *heavy), -bound, bound).astype(held_as)


def setup_inputs(seed: int = 0) -> dict:
    streams_of = jax.random.split(jax.random.key(seed), 10)
    x_late = scatter_about(streams_of[0], (TOKENS, D), 1.0, 6.0, ((0, 16),))
    x_early = scatter_about(streams_of[1], (TOKENS, D), 1.0, 6.0, ((0, 16),))
    cotangent = bell_draw_with(streams_of[2], (TOKENS, D), 1.0, 6.0, ((0, 16),), (0, 1, 16, 2.0))
    w_gate = scatter_about(streams_of[3], (D, FF), D ** -0.5, 0.125, ((0, 16), (1, 2)))
    w_up = scatter_about(streams_of[4], (D, FF), D ** -0.5, 0.125, ((0, 16), (1, 2)))
    w_down = scatter_about(streams_of[5], (FF, D), FF ** -0.5, 0.09375, ((0, 2), (1, 16)))
    conv_taps = scatter_about(streams_of[6], (TAPS, FF), 0.6, 3.0, (), jnp.float32)
    conv_bias = scatter_about(streams_of[7], (FF,), 0.5, 3.0, (), jnp.float32)
    grad_down = scatter_about(streams_of[8], (FF, D), 10.0, 60.0, ((0, 2), (1, 16)), jnp.float32)
    return {"x_late": x_late, "x_early": x_early, "cotangent": cotangent, "w_gate": w_gate, "w_up": w_up, "w_down": w_down, "conv_taps": conv_taps, "conv_bias": conv_bias, "grad_down": grad_down}


def shift_later(field, steps):
    pad = jnp.zeros((field.shape[0], steps, field.shape[2]), jnp.float32)
    return jnp.concatenate([pad, field[:, :field.shape[1] - steps]], axis=1)


def shift_earlier(field, steps):
    pad = jnp.zeros((field.shape[0], steps, field.shape[2]), jnp.float32)
    return jnp.concatenate([field[:, steps:], pad], axis=1)


def mlp_parts(inputs, w_gate, w_up, conv_taps, conv_bias):
    gate = jnp.dot(inputs, w_gate, preferred_element_type=jnp.float32).astype(jnp.bfloat16)
    up = jnp.dot(inputs, w_up, preferred_element_type=jnp.float32)
    seqs = gate.astype(jnp.float32).reshape(N_FS, TOK_DEV, FF)
    conv = conv_bias + conv_taps[2] * seqs + conv_taps[1] * shift_later(seqs, 1) + conv_taps[0] * shift_later(seqs, 2)
    conv = conv.reshape(TOKENS, FF)
    act = jax.nn.silu(conv)
    hidden = (act * up).astype(jnp.bfloat16)
    return conv, act, up, hidden


def rounded(value):
    return lax.optimization_barrier(value.astype(jnp.bfloat16)).astype(jnp.float32)


def reference(x_late, x_early, cotangent, w_gate, w_up, w_down, conv_taps, conv_bias, grad_down):
    width = FF // N_TP
    conv, act, up, hidden = mlp_parts(x_late, w_gate, w_up, conv_taps, conv_bias)
    total = jnp.zeros((TOKENS, D), jnp.float32)
    for block in range(N_TP):
        lo = block * width
        total = total + rounded(jnp.dot(hidden[:, lo:lo + width], w_down[lo:lo + width], preferred_element_type=jnp.float32))
    y_late = total.astype(jnp.bfloat16)

    conv, act, up, hidden = mlp_parts(x_early, w_gate, w_up, conv_taps, conv_bias)
    dhidden = jnp.dot(cotangent, w_down.T, preferred_element_type=jnp.float32)
    dup = (dhidden * act).astype(jnp.bfloat16)
    sig = jax.nn.sigmoid(conv)
    dconv = (dhidden * up * sig * (1.0 + conv * (1.0 - sig))).reshape(N_FS, TOK_DEV, FF)
    dgate = conv_taps[2] * dconv + conv_taps[1] * shift_earlier(dconv, 1) + conv_taps[0] * shift_earlier(dconv, 2)
    dgate = dgate.reshape(TOKENS, FF).astype(jnp.bfloat16)
    total = jnp.zeros((TOKENS, D), jnp.float32)
    for block in range(N_TP):
        lo = block * width
        part = jnp.dot(dup[:, lo:lo + width], w_up[:, lo:lo + width].T, preferred_element_type=jnp.float32)
        part = part + jnp.dot(dgate[:, lo:lo + width], w_gate[:, lo:lo + width].T, preferred_element_type=jnp.float32)
        total = total + rounded(part)
    dx_early = total.astype(jnp.bfloat16)
    grad_down_out = grad_down + jnp.dot(hidden.T, cotangent, preferred_element_type=jnp.float32)
    return y_late, dx_early, grad_down_out
```

```python
import functools

import jax
import jax.numpy as jnp
from jax import lax
from jax.experimental import pallas as pl
from jax.experimental.pallas import tpu as pltpu
from jax.sharding import PartitionSpec as P

GROUP = 4
VMEM_BYTES = 60 * 1024 * 1024
ANY = pl.BlockSpec(memory_space=pl.ANY)
VMEM = pl.BlockSpec(memory_space=pltpu.VMEM)


def place():
    f, c = lax.axis_index("fs"), lax.axis_index("tp")
    q, z = lax.rem(f, GROUP), lax.div(f, GROUP)
    qx = q + 1 - 2 * lax.rem(q, 2)
    qy = q + 2 - 4 * lax.div(q, 2)
    qa, qb = qx + c * (qy - qx), qy + c * (qx - qy)
    return f, c, q, z, qa, qb, GROUP - 1 - q


def at(start, size):
    return pl.ds(pl.multiple_of(start, size), size)


def remote(src, dst, send, recv, **device):
    return pltpu.make_async_remote_copy(
        src_ref=src, dst_ref=dst, send_sem=send, recv_sem=recv,
        device_id=device, device_id_type=pl.DeviceIdType.MESH,
    )


def gather_kernel(nz, x0, x1, x2, wg, wu, wd, t0, t1, t2, og, ou, od,
                  loc, w_s, w_r, n_s, n_r, p_s, p_r, r_s, r_r, l_s, l_r):
    f, c, q, z, qa, qb, qd = place()
    base = z * GROUP
    xs, ts, outs = (x0, x1, x2), (t0, t1, t2), (og, ou, od)
    rows = x0.shape[0]
    half = rows // 2
    r, u = wg.shape[0], og.shape[1]
    first, last = z > 0, z < nz - 1

    barrier = pltpu.get_barrier_semaphore()
    for peer in (qa, qb, qd):
        pl.semaphore_signal(barrier, 1, device_id={"fs": base + peer}, device_id_type=pl.DeviceIdType.MESH)
    pl.semaphore_signal(barrier, 1, device_id={"tp": 1 - c}, device_id_type=pl.DeviceIdType.MESH)

    for s in range(1, nz):
        pl.semaphore_signal(barrier, 1, device_id={"fs": lax.rem(z + s, nz) * GROUP + q},
                            device_id_type=pl.DeviceIdType.MESH)
    pl.semaphore_wait(barrier, 3 + nz)

    def piece(k, peer):
        if k == 2:
            return wd.at[at(peer * u, u), :]
        return (wg, wu)[k].at[:, at(peer * u, u)]

    def landing(k, owner):
        if k == 2:
            return od.at[:, at(owner * r, r)]
        return outs[k].at[at(owner * r, r), :]

    weights = []
    for k in range(3):
        for d, peer in enumerate((qa, qb, qd)):
            copy = remote(piece(k, peer), landing(k, f), w_s.at[k, d], w_r.at[k, d], fs=base + peer)
            copy.start()
            weights.append(copy)
    mine = at(c * half, half)
    near = []
    for i in range(3):
        for d, peer in enumerate((qa, qb)):
            copy = remote(xs[i].at[mine, :], ts[i].at[q, mine, :], n_s.at[i, d], n_r.at[i, d], fs=base + peer)
            copy.start()
            near.append(copy)
    local = []
    for k in range(3):
        copy = pltpu.make_async_copy(piece(k, q), landing(k, f), loc.at[k])
        copy.start()
        local.append(copy)
    for i in range(3):
        copy = pltpu.make_async_copy(xs[i], ts[i].at[q], loc.at[3 + i])
        copy.start()
        local.append(copy)

    def block(k, b):
        if k == 2:
            return od.at[:, at(b * GROUP * r, GROUP * r)]
        return outs[k].at[at(b * GROUP * r, GROUP * r), :]

    def right(k, s):
        b = block(k, z - s)
        return remote(b, b, r_s.at[s, k], r_r.at[s, k], fs=f + GROUP)

    def left(k, s):
        b = block(k, z + s)
        return remote(b, b, l_s.at[s, k], l_r.at[s, k], fs=f - GROUP)

    def arrived(k, s):
        @pl.when(z - s - 1 >= 0)
        def _():
            b = block(k, z - s - 1)
            remote(b, b, r_s.at[s, k], r_r.at[s, k], fs=f - GROUP).wait_recv()

        @pl.when(z + s + 1 < nz)
        def _():
            b = block(k, z + s + 1)
            remote(b, b, l_s.at[s, k], l_r.at[s, k], fs=f + GROUP).wait_recv()

    def onward(k, s, act):
        @pl.when(jnp.logical_and(z - s >= 0, last))
        def _():
            act(right(k, s))

        @pl.when(jnp.logical_and(z + s < nz, first))
        def _():
            act(left(k, s))

    begin, sent = (lambda copy: copy.start()), (lambda copy: copy.wait_send())

    for k in range(3):
        local[k].wait()
        for d in range(3):
            weights[3 * k + d].wait_recv()
        onward(k, 0, begin)

    partner = []

    def pass_on(i, owner, kind):
        there = ts[i].at[owner, mine, :]
        copy = remote(there, there, p_s.at[i, kind], p_r.at[i, kind], tp=1 - c)
        copy.start()
        partner.append((copy, i, owner, kind))

    far = []
    for i in range(3):
        near[2 * i].wait_recv()
        there = ts[i].at[qa, mine, :]
        copy = remote(there, there, n_s.at[i, 2], n_r.at[i, 2], fs=base + qb)
        copy.start()
        far.append(copy)
        pass_on(i, qa, 0)
        if nz > 2:
            arrived(i, 0)
            onward(i, 1, begin)
    for i in range(3):
        near[2 * i + 1].wait_recv()
        pass_on(i, qb, 1)
    for i in range(3):
        far[i].wait_recv()
        pass_on(i, qd, 2)
    for s in range(2, nz - 1):
        for k in range(3):
            arrived(k, s - 1)
            onward(k, s, begin)
    for k in range(3):
        if nz > 1:
            arrived(k, nz - 2)
    other = at((1 - c) * half, half)
    for copy, i, owner, kind in partner:
        copy.wait_send()
        theirs = (qb, qa, qd)[kind]
        there = ts[i].at[theirs, other, :]
        remote(there, there, p_s.at[i, kind], p_r.at[i, kind], tp=1 - c).wait_recv()
    for copy in weights + near + far:
        copy.wait_send()
    for copy in local[3:]:
        copy.wait()
    for s in range(nz - 1):
        for k in range(3):
            onward(k, s, sent)


def gather(nz, xs, w_gate, w_up, w_down):
    rows, d = xs[0].shape
    units = w_gate.shape[1] // GROUP
    dma = pltpu.SemaphoreType.DMA
    hops = max(nz - 1, 1)
    tok = jax.ShapeDtypeStruct((GROUP, rows, d), xs[0].dtype)
    col = jax.ShapeDtypeStruct((d, units), w_gate.dtype)
    row = jax.ShapeDtypeStruct((units, d), w_gate.dtype)
    return pl.pallas_call(
        functools.partial(gather_kernel, nz),
        out_shape=(tok, tok, tok, col, col, row),
        in_specs=[VMEM] * 6,
        out_specs=(ANY,) * 6,
        scratch_shapes=[dma((6,)), dma((3, 3)), dma((3, 3)), dma((3, 3)), dma((3, 3)),
                        dma((3, 3)), dma((3, 3)), dma((hops, 3)), dma((hops, 3)),
                        dma((hops, 3)), dma((hops, 3))],
        compiler_params=pltpu.CompilerParams(collective_id=0, has_side_effects=True, vmem_limit_bytes=VMEM_BYTES),
        name="gather_group",
    )(*xs, w_gate, w_up, w_down)


def total(dst, srcs, rows, step=16):
    @pl.loop(0, rows, step=step)
    def _(i):
        sl = pl.ds(pl.multiple_of(i, step), step)
        out = srcs[0][sl, :].astype(jnp.float32)
        for s in srcs[1:]:
            out = out + s[sl, :].astype(jnp.float32)
        dst[sl, :] = out.astype(dst.dtype)


def scatter_kernel(nz, yp, xp, gp, y, dx, g, core, summed, got, gin, gsum,
                   c_s, c_r, a_s, a_r, z_s, z_r, g_s, g_r, e_s, e_r):
    f, c, q, z, qa, qb, qd = place()
    base = z * GROUP
    parts, outs = (yp, xp), (y, dx)
    rows = y.shape[0]
    half = rows // 2
    u = gp.shape[0]
    r = g.shape[1]
    wide = GROUP * r

    barrier = pltpu.get_barrier_semaphore()
    for peer in (qa, qb, qd):
        pl.semaphore_signal(barrier, 1, device_id={"fs": base + peer}, device_id_type=pl.DeviceIdType.MESH)
    pl.semaphore_signal(barrier, 1, device_id={"tp": 1 - c}, device_id_type=pl.DeviceIdType.MESH)
    for s in range(1, nz):
        pl.semaphore_signal(barrier, 1, device_id={"fs": lax.rem(z + s, nz) * GROUP + q},
                            device_id_type=pl.DeviceIdType.MESH)
    pl.semaphore_wait(barrier, 3 + nz)

    order = (qd, qa, qb, q)
    theirs = (qd, qb, qa, q)
    cores = []
    for t in range(2):
        for n in range(4):
            src = parts[t].at[at(theirs[n] * rows + (1 - c) * half, half), :]
            copy = remote(src, core.at[t, n], c_s.at[t, n], c_r.at[t, n], tp=1 - c)
            copy.start()
            cores.append(copy)
    grads = []
    for s in range(1, nz):
        to = lax.rem(z + s, nz)
        copy = remote(gp.at[:, at(to * wide, wide)], gin.at[s], z_s.at[s], z_r.at[s], fs=to * GROUP + q)
        copy.start()
        grads.append(copy)

    sends = {}

    def send(t, n, slot, peer):
        copy = remote(summed.at[t, n], got.at[t, slot], a_s.at[t, slot], a_r.at[t, slot], fs=base + peer)
        copy.start()
        sends[t, slot] = copy

    for n in range(4):
        for t in range(2):
            cores[4 * t + n].wait_recv()
            own = parts[t].at[at(order[n] * rows + c * half, half), :]
            total(summed.at[t, n], [own, core.at[t, n]], half)
            if n == 0:
                send(t, 0, 0, qa)
            if n == 1:
                send(t, 1, 1, qa)
    for t in range(2):
        sends[t, 0].wait_recv()
        total(core.at[t, 0], [summed.at[t, 2], got.at[t, 0]], half)
        copy = remote(core.at[t, 0], got.at[t, 2], a_s.at[t, 2], a_r.at[t, 2], fs=base + qb)
        copy.start()
        sends[t, 2] = copy
    for copy in grads:
        copy.wait_recv()
    total(gsum, [gp.at[:, at(z * wide, wide)]] + [gin.at[s] for s in range(1, nz)], u)
    handed = []
    for d, peer in enumerate((qa, qb, qd)):
        copy = remote(gsum.at[:, at(peer * r, r)], g.at[at(q * u, u), :], g_s.at[d], g_r.at[d], fs=base + peer)
        copy.start()
        handed.append(copy)
    g[at(q * u, u), :] = gsum[:, at(q * r, r)]
    ends = []
    mine = at(c * half, half)
    for t in range(2):
        sends[t, 1].wait_recv()
        sends[t, 2].wait_recv()
        total(outs[t].at[mine, :], [summed.at[t, 3], got.at[t, 1], got.at[t, 2]], half)
        copy = remote(outs[t].at[mine, :], outs[t].at[mine, :], e_s.at[t], e_r.at[t], tp=1 - c)
        copy.start()
        ends.append(copy)
    for copy in handed + ends:
        copy.wait_recv()
    for copy in cores + grads + handed + ends + list(sends.values()):
        copy.wait_send()


def scatter(nz, y_part, dx_part, g_part):
    d = y_part.shape[1]
    rows = y_part.shape[0] // GROUP
    u = g_part.shape[0]
    r = d // (nz * GROUP)
    half = rows // 2
    dma = pltpu.SemaphoreType.DMA
    b16 = jnp.bfloat16
    out = jax.ShapeDtypeStruct((rows, d), b16)
    return pl.pallas_call(
        functools.partial(scatter_kernel, nz),
        out_shape=(out, out, jax.ShapeDtypeStruct((u * GROUP, r), b16)),
        in_specs=[VMEM] * 3,
        out_specs=(VMEM,) * 3,
        scratch_shapes=[
            pltpu.VMEM((2, 4, half, d), b16), pltpu.VMEM((2, 4, half, d), b16), pltpu.VMEM((2, 3, half, d), b16),
            pltpu.VMEM((nz, u, GROUP * r), b16), pltpu.VMEM((u, GROUP * r), b16),
            dma((2, 4)), dma((2, 4)), dma((2, 3)), dma((2, 3)), dma((nz,)), dma((nz,)),
            dma((3,)), dma((3,)), dma((2,)), dma((2,)),
        ],
        compiler_params=pltpu.CompilerParams(collective_id=1, has_side_effects=True, vmem_limit_bytes=VMEM_BYTES),
        name="scatter_group",
    )(y_part, dx_part, g_part)


def shift_later(field, steps):
    pad = jnp.zeros((steps, field.shape[1]), jnp.float32)
    return jnp.concatenate([pad, field[: field.shape[0] - steps]], axis=0)


def seq_later(field, steps, rows):
    row = lax.rem(lax.broadcasted_iota(jnp.int32, (field.shape[0], 1), 0), rows)
    return jnp.where(row >= steps, shift_later(field, steps), 0.0)


def seq_earlier(field, steps, rows):
    row = lax.rem(lax.broadcasted_iota(jnp.int32, (field.shape[0], 1), 0), rows)
    return jnp.where(row < rows - steps, shift_earlier(field, steps), 0.0)


def shift_earlier(field, steps):
    pad = jnp.zeros((steps, field.shape[1]), jnp.float32)
    return jnp.concatenate([field[steps:], pad], axis=0)


def contract_last(left, right):
    return lax.dot_general(
        left, right, (((1,), (1,)), ((), ())), preferred_element_type=jnp.float32
    )


def hidden_parts(inputs, gate_full, up_full, taps, bias, rows):
    gate = (
        jnp.dot(inputs, gate_full, preferred_element_type=jnp.float32)
        .astype(jnp.bfloat16)
        .astype(jnp.float32)
    )
    up = jnp.dot(inputs, up_full, preferred_element_type=jnp.float32)
    conv = bias + taps[2] * gate + taps[1] * seq_later(gate, 1, rows) + taps[0] * seq_later(gate, 2, rows)
    act = jax.nn.silu(conv)
    hidden = (act * up).astype(jnp.bfloat16)
    return (conv, act, up, hidden)


def forward_pass(x_late, gate_full, up_full, down_full, taps, bias):
    conv, act, up, hidden = hidden_parts(x_late, gate_full, up_full, taps, bias, x_late.shape[0])
    partial_value = jnp.dot(hidden, down_full, preferred_element_type=jnp.float32)
    return lax.psum(partial_value.astype(jnp.bfloat16), "tp")


def backward_pass(x_early, cotangent, gate_full, up_full, down_full, taps, bias, grad_down):
    conv, act, up, hidden = hidden_parts(x_early, gate_full, up_full, taps, bias, x_early.shape[0])
    dhidden = contract_last(cotangent, down_full)
    summed = lax.psum_scatter(
        lax.dot_general(
            cotangent, hidden, (((0,), (0,)), ((), ())), preferred_element_type=jnp.float32
        ),
        "fs",
        scatter_dimension=0,
        tiled=True,
    )
    grad_down_out = grad_down + summed.T
    dup = (dhidden * act).astype(jnp.bfloat16)
    sig = jax.nn.sigmoid(conv)
    dconv = dhidden * up * sig * (1.0 + conv * (1.0 - sig))
    dgate = taps[2] * dconv + taps[1] * shift_earlier(dconv, 1) + taps[0] * shift_earlier(dconv, 2)
    dgate = dgate.astype(jnp.bfloat16)
    partial_value = contract_last(dup, up_full) + contract_last(dgate, gate_full)
    dx_early = lax.psum(partial_value.astype(jnp.bfloat16), "tp")
    return (dx_early, grad_down_out)


def shards(x_late, x_early, cotangent, w_gate, w_up, w_down, conv_taps, conv_bias, grad_down):
    width = w_gate.shape[1]
    offset = lax.axis_index("tp") * width
    taps = lax.dynamic_slice_in_dim(conv_taps, offset, width, 1)
    bias = lax.dynamic_slice_in_dim(conv_bias, offset, width, 0)
    gate_full, up_full = (
        lax.all_gather(w_gate, "fs", axis=0, tiled=True),
        lax.all_gather(w_up, "fs", axis=0, tiled=True),
    )
    down_full = lax.all_gather(w_down, "fs", axis=1, tiled=True)
    y_late = forward_pass(x_late, gate_full, up_full, down_full, taps, bias)
    dx_early, grad_down_out = backward_pass(
        x_early, cotangent, gate_full, up_full, down_full, taps, bias, grad_down
    )
    return (y_late, dx_early, grad_down_out)


def grouped_shards(nz, x_late, x_early, cotangent, w_gate, w_up, w_down, conv_taps, conv_bias, grad_down):
    rows, d = x_late.shape
    units = w_gate.shape[1] // GROUP
    start = (lax.axis_index("tp") * GROUP + lax.rem(lax.axis_index("fs"), GROUP)) * units
    taps = lax.dynamic_slice_in_dim(conv_taps, start, units, 1)
    bias = lax.dynamic_slice_in_dim(conv_bias, start, units, 0)
    late, early, cot, gate_w, up_w, down_w = gather(nz, (x_late, x_early, cotangent), w_gate, w_up, w_down)
    late, early, cot = (t.reshape(GROUP * rows, d) for t in (late, early, cot))

    hidden = hidden_parts(late, gate_w, up_w, taps, bias, rows)[3]
    y_part = jnp.dot(hidden, down_w, preferred_element_type=jnp.float32).astype(jnp.bfloat16)

    conv, act, up, hidden = hidden_parts(early, gate_w, up_w, taps, bias, rows)
    g_part = lax.dot_general(
        hidden, cot, (((0,), (0,)), ((), ())), preferred_element_type=jnp.float32
    ).astype(jnp.bfloat16)
    dhidden = contract_last(cot, down_w)
    dup = (dhidden * act).astype(jnp.bfloat16)
    sig = jax.nn.sigmoid(conv)
    dconv = dhidden * up * sig * (1.0 + conv * (1.0 - sig))
    dgate = taps[2] * dconv + taps[1] * seq_earlier(dconv, 1, rows) + taps[0] * seq_earlier(dconv, 2, rows)
    dgate = dgate.astype(jnp.bfloat16)
    dx_part = (contract_last(dup, up_w) + contract_last(dgate, gate_w)).astype(jnp.bfloat16)

    y_late, dx_early, grad = scatter(nz, y_part, dx_part, g_part)
    return (y_late, dx_early, grad_down + grad.astype(jnp.float32))


def solution(mesh):
    def step(*arrays):
        x_late, w_gate = arrays[0], arrays[3]
        fs, tp = mesh.shape["fs"], mesh.shape["tp"]
        units, rest = divmod(w_gate.shape[1], GROUP)
        lanes_ok = rest == 0 and units % 128 == 0 and w_gate.shape[0] % 128 == 0
        if tp == 2 and fs % GROUP == 0 and lanes_ok and x_late.shape[0] % 32 == 0:
            return grouped_shards(fs // GROUP, *arrays)
        return shards(*arrays)

    placed = (
        P("fs", None),
        P("fs", None),
        P("fs", None),
        P("fs", "tp"),
        P("fs", "tp"),
        P("tp", "fs"),
        P(),
        P(),
        P("tp", "fs"),
    )
    return jax.shard_map(
        step,
        mesh=mesh,
        in_specs=placed,
        out_specs=(P("fs", None), P("fs", None), P("tp", "fs")),
        check_vma=False,
    )
```

```python
import functools

import jax
import jax.numpy as jnp
from jax import lax
from jax.experimental import pallas as pl
from jax.experimental.pallas import tpu as pltpu
from jax.sharding import PartitionSpec as P

GROUP = 4
VMEM_BYTES = 60 * 1024 * 1024
VMEM = pl.BlockSpec(memory_space=pltpu.VMEM)


def place():
    f, c = lax.axis_index("fs"), lax.axis_index("tp")
    q, z = lax.rem(f, GROUP), lax.div(f, GROUP)
    qx = q + 1 - 2 * lax.rem(q, 2)
    qy = q + 2 - 4 * lax.div(q, 2)
    qa, qb = qx + c * (qy - qx), qy + c * (qx - qy)
    return f, c, q, z, qa, qb, GROUP - 1 - q


def at(start, size):
    return pl.ds(pl.multiple_of(start, size), size)


def remote(src, dst, send, recv, **device):
    return pltpu.make_async_remote_copy(
        src_ref=src, dst_ref=dst, send_sem=send, recv_sem=recv,
        device_id=device, device_id_type=pl.DeviceIdType.MESH,
    )


def total(dst, srcs, rows, step=16):
    @pl.loop(0, rows, step=step)
    def _(i):
        sl = pl.ds(pl.multiple_of(i, step), step)
        out = srcs[0][sl, :].astype(jnp.float32)
        for s in srcs[1:]:
            out = out + s[sl, :].astype(jnp.float32)
        dst[sl, :] = out.astype(dst.dtype)


def mm(left, right, dims=((1,), (0,))):
    return lax.dot_general(left, right, (dims, ((), ())), preferred_element_type=jnp.float32)


def layer_kernel(nz, tile, x0, x1, x2, wg, wu, wd, taps, bias, y, dx, g,
                 t0, t1, t2, og, ou, od, hid, hid_t, conv_s, up_s, dup, dgate, yp, xp, gp,
                 core, summed, got, gin, gsum,
                 loc, w_s, w_r, n_s, n_r, p_s, p_r, r_s, r_r, l_s, l_r,
                 c_s, c_r, a_s, a_r, z_s, z_r, g_s, g_r, e_s, e_r):
    f, c, q, z, qa, qb, qd = place()
    base = z * GROUP
    xs, ts, outs = (x0, x1, x2), (t0, t1, t2), (og, ou, od)
    rows, d_model = x0.shape
    half = rows // 2
    r, u = wg.shape[0], og.shape[1]
    wide = GROUP * r
    first, last = z > 0, z < nz - 1

    barrier = pltpu.get_barrier_semaphore()
    for peer in (qa, qb, qd):
        pl.semaphore_signal(barrier, 1, device_id={"fs": base + peer}, device_id_type=pl.DeviceIdType.MESH)
    pl.semaphore_signal(barrier, 1, device_id={"tp": 1 - c}, device_id_type=pl.DeviceIdType.MESH)

    for s in range(1, nz):
        pl.semaphore_signal(barrier, 1, device_id={"fs": lax.rem(z + s, nz) * GROUP + q},
                            device_id_type=pl.DeviceIdType.MESH)
    pl.semaphore_wait(barrier, 3 + nz)

    def piece(k, peer):
        if k == 2:
            return wd.at[at(peer * u, u), :]
        return (wg, wu)[k].at[:, at(peer * u, u)]

    def landing(k, owner):
        if k == 2:
            return od.at[:, at(owner * r, r)]
        return outs[k].at[at(owner * r, r), :]

    weights = []
    for k in range(3):
        for d, peer in enumerate((qa, qb, qd)):
            copy = remote(piece(k, peer), landing(k, f), w_s.at[k, d], w_r.at[k, d], fs=base + peer)
            copy.start()
            weights.append(copy)
    mine = at(c * half, half)
    near = []
    for i in range(3):
        for d, peer in enumerate((qa, qb)):
            copy = remote(xs[i].at[mine, :], ts[i].at[q, mine, :], n_s.at[i, d], n_r.at[i, d], fs=base + peer)
            copy.start()
            near.append(copy)
    local = []
    for k in range(3):
        copy = pltpu.make_async_copy(piece(k, q), landing(k, f), loc.at[k])
        copy.start()
        local.append(copy)
    for i in range(3):
        copy = pltpu.make_async_copy(xs[i], ts[i].at[q], loc.at[3 + i])
        copy.start()
        local.append(copy)

    def block(k, b):
        if k == 2:
            return od.at[:, at(b * GROUP * r, GROUP * r)]
        return outs[k].at[at(b * GROUP * r, GROUP * r), :]

    def right(k, s):
        b = block(k, z - s)
        return remote(b, b, r_s.at[s, k], r_r.at[s, k], fs=f + GROUP)

    def left(k, s):
        b = block(k, z + s)
        return remote(b, b, l_s.at[s, k], l_r.at[s, k], fs=f - GROUP)

    def arrived(k, s):
        @pl.when(z - s - 1 >= 0)
        def _():
            b = block(k, z - s - 1)
            remote(b, b, r_s.at[s, k], r_r.at[s, k], fs=f - GROUP).wait_recv()

        @pl.when(z + s + 1 < nz)
        def _():
            b = block(k, z + s + 1)
            remote(b, b, l_s.at[s, k], l_r.at[s, k], fs=f + GROUP).wait_recv()

    def onward(k, s, act):
        @pl.when(jnp.logical_and(z - s >= 0, last))
        def _():
            act(right(k, s))

        @pl.when(jnp.logical_and(z + s < nz, first))
        def _():
            act(left(k, s))

    begin, sent = (lambda copy: copy.start()), (lambda copy: copy.wait_send())

    row = lax.broadcasted_iota(jnp.int32, (rows, tile), 0)

    def later(v, steps):
        return jnp.where(row >= steps, pltpu.roll(v, steps, 0), 0.0)

    def earlier(v, steps):
        return jnp.where(row < rows - steps, pltpu.roll(v, rows - steps, 0), 0.0)

    def forward(t, keep):
        @pl.loop(0, GROUP)
        def _(b):
            @pl.loop(0, u // tile)
            def _(j):
                cols, seq = at(j * tile, tile), at(b * rows, rows)
                x = t[b]
                gate = mm(x, og[:, cols]).astype(jnp.bfloat16).astype(jnp.float32)
                up = mm(x, ou[:, cols])
                conv = (bias[:, cols] + taps[2:3, cols] * gate + taps[1:2, cols] * later(gate, 1)
                        + taps[0:1, cols] * later(gate, 2))
                out = conv / (1.0 + jnp.exp(-conv)) * up
                if keep:
                    conv_s[seq, cols] = conv
                    up_s[seq, cols] = up
                    hid_t[at(j * tile, tile), seq] = out.T.astype(jnp.bfloat16)
                else:
                    hid[seq, cols] = out.astype(jnp.bfloat16)

    def down_grad():
        @pl.loop(0, d_model // tile)
        def _(j):
            cols = at(j * tile, tile)
            cot = t2[:, :, cols].reshape(GROUP * rows, tile)
            gp[:, cols] = mm(hid_t[...], cot).astype(jnp.bfloat16)

    def backward():
        @pl.loop(0, GROUP)
        def _(b):
            @pl.loop(0, u // tile)
            def _(j):
                cols, seq = at(j * tile, tile), at(b * rows, rows)
                dh = mm(t2[b], od[at(j * tile, tile), :], ((1,), (1,)))
                conv = conv_s[seq, cols]
                sig = 1.0 / (1.0 + jnp.exp(-conv))
                dup[seq, cols] = (dh * (conv * sig)).astype(jnp.bfloat16)
                dc = dh * up_s[seq, cols] * sig * (1.0 + conv * (1.0 - sig))
                dg = (taps[2:3, cols] * dc + taps[1:2, cols] * earlier(dc, 1)
                      + taps[0:1, cols] * earlier(dc, 2))
                dgate[seq, cols] = dg.astype(jnp.bfloat16)

    def late_out(owner):
        seq = at(owner * rows, rows)

        @pl.loop(0, d_model // tile)
        def _(j):
            cols = at(j * tile, tile)
            yp[seq, cols] = mm(hid[seq, :], od[:, cols]).astype(jnp.bfloat16)

    def early_out(owner):
        seq = at(owner * rows, rows)

        @pl.loop(0, d_model // tile)
        def _(j):
            cols = at(j * tile, tile)
            part = mm(dup[seq, :], ou[cols, :], ((1,), (1,))) + mm(dgate[seq, :], og[cols, :], ((1,), (1,)))
            xp[seq, cols] = part.astype(jnp.bfloat16)

    def enter(k):
        local[k].wait()
        for d in range(3):
            weights[3 * k + d].wait_recv()
        onward(k, 0, begin)

    enter(0)
    enter(1)
    partner = []

    def pass_on(i, owner, kind):
        there = ts[i].at[owner, mine, :]
        copy = remote(there, there, p_s.at[i, kind], p_r.at[i, kind], tp=1 - c)
        copy.start()
        partner.append((copy, i, owner, kind))

    far = []
    for i in range(3):
        near[2 * i].wait_recv()
        there = ts[i].at[qa, mine, :]
        copy = remote(there, there, n_s.at[i, 2], n_r.at[i, 2], fs=base + qb)
        copy.start()
        far.append(copy)
        pass_on(i, qa, 0)
        if i < 2 and nz > 2:
            arrived(i, 0)
            onward(i, 1, begin)
    for i in range(3):
        near[2 * i + 1].wait_recv()
        pass_on(i, qb, 1)
    for s in range(2, nz - 1):
        for k in range(2):
            arrived(k, s - 1)
            onward(k, s, begin)
    enter(2)
    for i in range(3):
        far[i].wait_recv()
        pass_on(i, qd, 2)
    if nz > 1:
        arrived(0, nz - 2)
        arrived(1, nz - 2)
    other = at((1 - c) * half, half)
    for copy, i, owner, kind in partner:
        there = ts[i].at[(qb, qa, qd)[kind], other, :]
        remote(there, there, p_s.at[i, kind], p_r.at[i, kind], tp=1 - c).wait_recv()
    for copy in local[3:]:
        copy.wait()

    jobs = [lambda: forward(t1, True), lambda: forward(t0, False), down_grad]
    for s in range(1, nz - 1):
        if jobs:
            jobs.pop(0)()
        arrived(2, s - 1)
        onward(2, s, begin)
    while jobs:
        jobs.pop(0)()
    grads = []
    for s in range(1, nz):
        to = lax.rem(z + s, nz)
        copy = remote(gp.at[:, at(to * wide, wide)], gin.at[s], z_s.at[s], z_r.at[s], fs=to * GROUP + q)
        copy.start()
        grads.append(copy)
    if nz > 1:
        arrived(2, nz - 2)

    parts, finals = (yp, xp), (y, dx)
    order = (qd, qa, qb, q)
    theirs = (qd, qb, qa, q)
    cores, sends = {}, {}

    def to_core(t, n):
        src = parts[t].at[at(theirs[n] * rows + (1 - c) * half, half), :]
        copy = remote(src, core.at[t, n], c_s.at[t, n], c_r.at[t, n], tp=1 - c)
        copy.start()
        cores[t, n] = copy

    def send(t, n, slot, peer):
        copy = remote(summed.at[t, n], got.at[t, slot], a_s.at[t, slot], a_r.at[t, slot], fs=base + peer)
        copy.start()
        sends[t, slot] = copy

    def join(t, n):
        cores[t, n].wait_recv()
        own = parts[t].at[at(order[n] * rows + c * half, half), :]
        total(summed.at[t, n], [own, core.at[t, n]], half)
        if n == 0:
            send(t, 0, 0, qa)
        if n == 1:
            send(t, 1, 1, qa)

    def onto_second(t):
        sends[t, 0].wait_recv()
        total(core.at[t, 0], [summed.at[t, 2], got.at[t, 0]], half)
        copy = remote(core.at[t, 0], got.at[t, 2], a_s.at[t, 2], a_r.at[t, 2], fs=base + qb)
        copy.start()
        sends[t, 2] = copy

    ends = []

    def finish(t):
        sends[t, 1].wait_recv()
        sends[t, 2].wait_recv()
        total(finals[t].at[mine, :], [summed.at[t, 3], got.at[t, 1], got.at[t, 2]], half)
        there = finals[t].at[mine, :]
        copy = remote(there, there, e_s.at[t], e_r.at[t], tp=1 - c)
        copy.start()
        ends.append(copy)

    def produce(t, make):
        make(qd)
        to_core(t, 0)
        make(qa)
        make(qb)
        to_core(t, 1)
        to_core(t, 2)
        join(t, 0)
        make(q)
        to_core(t, 3)
        for n in (1, 2):
            join(t, n)

    produce(0, late_out)
    backward()
    join(0, 3)
    onto_second(0)
    produce(1, early_out)
    join(1, 3)
    finish(0)
    onto_second(1)
    for copy in grads:
        copy.wait_recv()
    total(gsum, [gp.at[:, at(z * wide, wide)]] + [gin.at[s] for s in range(1, nz)], u)
    handed = []
    for d, peer in enumerate((qa, qb, qd)):
        copy = remote(gsum.at[:, at(peer * r, r)], g.at[at(q * u, u), :], g_s.at[d], g_r.at[d], fs=base + peer)
        copy.start()
        handed.append(copy)
    g[at(q * u, u), :] = gsum[:, at(q * r, r)]
    finish(1)
    for copy in handed + ends:
        copy.wait_recv()
    for copy in weights + near + far + [p[0] for p in partner]:
        copy.wait_send()
    for copy in list(cores.values()) + grads + handed + ends + list(sends.values()):
        copy.wait_send()
    for s in range(nz - 1):
        for k in range(3):
            onward(k, s, sent)


def layer(nz, xs, w_gate, w_up, w_down, taps, bias):
    rows, d = xs[0].shape
    u = w_gate.shape[1] // GROUP
    r = w_gate.shape[0]
    half, toks = rows // 2, GROUP * rows
    tile = 256 if u % 256 == 0 else 128
    sems = lambda *shape: [pltpu.SemaphoreType.DMA(shape)] * 2
    b16, f32 = jnp.bfloat16, jnp.float32
    out = jax.ShapeDtypeStruct((rows, d), b16)
    hops = max(nz - 1, 1)
    return pl.pallas_call(
        functools.partial(layer_kernel, nz, tile),
        out_shape=(out, out, jax.ShapeDtypeStruct((u * GROUP, r), b16)),
        in_specs=[VMEM] * 8,
        out_specs=(VMEM,) * 3,
        scratch_shapes=[pltpu.VMEM((GROUP, rows, d), b16)] * 3
        + [pltpu.VMEM((d, u), b16)] * 2
        + [pltpu.VMEM((u, d), b16), pltpu.VMEM((toks, u), b16), pltpu.VMEM((u, toks), b16),
           pltpu.VMEM((toks, u), f32), pltpu.VMEM((toks, u), f32),
           pltpu.VMEM((toks, u), b16), pltpu.VMEM((toks, u), b16),
           pltpu.VMEM((toks, d), b16), pltpu.VMEM((toks, d), b16), pltpu.VMEM((u, d), b16),
           pltpu.VMEM((2, 4, half, d), b16), pltpu.VMEM((2, 4, half, d), b16), pltpu.VMEM((2, 3, half, d), b16),
           pltpu.VMEM((nz, u, GROUP * r), b16), pltpu.VMEM((u, GROUP * r), b16),
           pltpu.SemaphoreType.DMA((6,))]
        + sems(3, 3) + sems(3, 3) + sems(3, 3) + sems(hops, 3) + sems(hops, 3)
        + sems(2, 4) + sems(2, 3) + sems(nz) + sems(3) + sems(2),
        compiler_params=pltpu.CompilerParams(collective_id=0, has_side_effects=True, vmem_limit_bytes=VMEM_BYTES),
        name="layer_group",
    )(*xs, w_gate, w_up, w_down, taps, bias)


def shift_later(field, steps):
    pad = jnp.zeros((steps, field.shape[1]), jnp.float32)
    return jnp.concatenate([pad, field[: field.shape[0] - steps]], axis=0)


def shift_earlier(field, steps):
    pad = jnp.zeros((steps, field.shape[1]), jnp.float32)
    return jnp.concatenate([field[steps:], pad], axis=0)


def contract_last(left, right):
    return lax.dot_general(
        left, right, (((1,), (1,)), ((), ())), preferred_element_type=jnp.float32
    )


def hidden_parts(inputs, gate_full, up_full, taps, bias):
    gate = (
        jnp.dot(inputs, gate_full, preferred_element_type=jnp.float32)
        .astype(jnp.bfloat16)
        .astype(jnp.float32)
    )
    up = jnp.dot(inputs, up_full, preferred_element_type=jnp.float32)
    conv = bias + taps[2] * gate + taps[1] * shift_later(gate, 1) + taps[0] * shift_later(gate, 2)
    act = jax.nn.silu(conv)
    hidden = (act * up).astype(jnp.bfloat16)
    return (conv, act, up, hidden)


def forward_pass(x_late, gate_full, up_full, down_full, taps, bias):
    conv, act, up, hidden = hidden_parts(x_late, gate_full, up_full, taps, bias)
    partial_value = jnp.dot(hidden, down_full, preferred_element_type=jnp.float32)
    return lax.psum(partial_value.astype(jnp.bfloat16), "tp")


def backward_pass(x_early, cotangent, gate_full, up_full, down_full, taps, bias, grad_down):
    conv, act, up, hidden = hidden_parts(x_early, gate_full, up_full, taps, bias)
    dhidden = contract_last(cotangent, down_full)
    summed = lax.psum_scatter(
        lax.dot_general(
            cotangent, hidden, (((0,), (0,)), ((), ())), preferred_element_type=jnp.float32
        ),
        "fs",
        scatter_dimension=0,
        tiled=True,
    )
    grad_down_out = grad_down + summed.T
    dup = (dhidden * act).astype(jnp.bfloat16)
    sig = jax.nn.sigmoid(conv)
    dconv = dhidden * up * sig * (1.0 + conv * (1.0 - sig))
    dgate = taps[2] * dconv + taps[1] * shift_earlier(dconv, 1) + taps[0] * shift_earlier(dconv, 2)
    dgate = dgate.astype(jnp.bfloat16)
    partial_value = contract_last(dup, up_full) + contract_last(dgate, gate_full)
    dx_early = lax.psum(partial_value.astype(jnp.bfloat16), "tp")
    return (dx_early, grad_down_out)


def shards(x_late, x_early, cotangent, w_gate, w_up, w_down, conv_taps, conv_bias, grad_down):
    width = w_gate.shape[1]
    offset = lax.axis_index("tp") * width
    taps = lax.dynamic_slice_in_dim(conv_taps, offset, width, 1)
    bias = lax.dynamic_slice_in_dim(conv_bias, offset, width, 0)
    gate_full, up_full = (
        lax.all_gather(w_gate, "fs", axis=0, tiled=True),
        lax.all_gather(w_up, "fs", axis=0, tiled=True),
    )
    down_full = lax.all_gather(w_down, "fs", axis=1, tiled=True)
    y_late = forward_pass(x_late, gate_full, up_full, down_full, taps, bias)
    dx_early, grad_down_out = backward_pass(
        x_early, cotangent, gate_full, up_full, down_full, taps, bias, grad_down
    )
    return (y_late, dx_early, grad_down_out)


def grouped_shards(nz, x_late, x_early, cotangent, w_gate, w_up, w_down, conv_taps, conv_bias, grad_down):
    units = w_gate.shape[1] // GROUP
    start = (lax.axis_index("tp") * GROUP + lax.rem(lax.axis_index("fs"), GROUP)) * units
    taps = lax.dynamic_slice_in_dim(conv_taps, start, units, 1)
    bias = lax.dynamic_slice_in_dim(conv_bias, start, units, 0)
    y_late, dx_early, grad = layer(
        nz, (x_late, x_early, cotangent), w_gate, w_up, w_down, taps, bias.reshape(1, units)
    )
    return (y_late, dx_early, grad_down + grad.astype(jnp.float32))


def solution(mesh):
    def step(*arrays):
        x_late, w_gate = arrays[0], arrays[3]
        fs, tp = mesh.shape["fs"], mesh.shape["tp"]
        units, rest = divmod(w_gate.shape[1], GROUP)
        lanes_ok = rest == 0 and units % 128 == 0 and w_gate.shape[0] % 128 == 0
        if tp == 2 and fs % GROUP == 0 and lanes_ok and x_late.shape[0] % 32 == 0:
            return grouped_shards(fs // GROUP, *arrays)
        return shards(*arrays)

    placed = (
        P("fs", None),
        P("fs", None),
        P("fs", None),
        P("fs", "tp"),
        P("fs", "tp"),
        P("tp", "fs"),
        P(),
        P(),
        P("tp", "fs"),
    )
    return jax.shard_map(
        step,
        mesh=mesh,
        in_specs=placed,
        out_specs=(P("fs", None), P("fs", None), P("tp", "fs")),
        check_vma=False,
    )
```

```python
import functools

import jax
import jax.numpy as jnp
from jax import lax
from jax.experimental import pallas as pl
from jax.experimental.pallas import tpu as pltpu
from jax.sharding import PartitionSpec as P

GROUP = 4
VMEM_BYTES = 60 * 1024 * 1024
VMEM = pl.BlockSpec(memory_space=pltpu.VMEM)


def place():
    f, c = lax.axis_index("fs"), lax.axis_index("tp")
    q, z = lax.rem(f, GROUP), lax.div(f, GROUP)
    qx = q + 1 - 2 * lax.rem(q, 2)
    qy = q + 2 - 4 * lax.div(q, 2)
    qa, qb = qx + c * (qy - qx), qy + c * (qx - qy)
    return f, c, q, z, qa, qb, GROUP - 1 - q


def at(start, size):
    return pl.ds(pl.multiple_of(start, size), size)


def remote(src, dst, send, recv, **device):
    return pltpu.make_async_remote_copy(
        src_ref=src, dst_ref=dst, send_sem=send, recv_sem=recv,
        device_id=device, device_id_type=pl.DeviceIdType.MESH,
    )


def total(dst, srcs, rows, step=16):
    @pl.loop(0, rows, step=step)
    def _(i):
        sl = pl.ds(pl.multiple_of(i, step), step)
        out = srcs[0][sl, :].astype(jnp.float32)
        for s in srcs[1:]:
            out = out + s[sl, :].astype(jnp.float32)
        dst[sl, :] = out.astype(dst.dtype)


def mm(left, right, dims=((1,), (0,))):
    return lax.dot_general(left, right, (dims, ((), ())), preferred_element_type=jnp.float32)


def layer_kernel(nz, tile, x0, x1, x2, wg, wu, wd, taps, bias, y, dx, g,
                 t0, t1, t2, og, ou, od, hid, hid_t, conv_s, up_s, dup, dgate, yp, xp, gp,
                 core, summed, got, gin, gsum,
                 loc, w_s, w_r, n_s, n_r, p_s, p_r, r_s, r_r, l_s, l_r,
                 c_s, c_r, a_s, a_r, z_s, z_r, g_s, g_r, e_s, e_r):
    f, c, q, z, qa, qb, qd = place()
    base = z * GROUP
    xs, ts, outs = (x0, x1, x2), (t0, t1, t2), (og, ou, od)
    rows, d_model = x0.shape
    half = rows // 2
    r, u = wg.shape[0], og.shape[1]
    wide = GROUP * r
    first, last = z > 0, z < nz - 1

    barrier = pltpu.get_barrier_semaphore()
    for peer in (qa, qb, qd):
        pl.semaphore_signal(barrier, 1, device_id={"fs": base + peer}, device_id_type=pl.DeviceIdType.MESH)
    pl.semaphore_signal(barrier, 1, device_id={"tp": 1 - c}, device_id_type=pl.DeviceIdType.MESH)

    for s in range(1, nz):
        pl.semaphore_signal(barrier, 1, device_id={"fs": lax.rem(z + s, nz) * GROUP + q},
                            device_id_type=pl.DeviceIdType.MESH)
    pl.semaphore_wait(barrier, 3 + nz)

    def piece(k, peer):
        if k == 2:
            return wd.at[at(peer * u, u), :]
        return (wg, wu)[k].at[:, at(peer * u, u)]

    def landing(k, owner):
        if k == 2:
            return od.at[:, at(owner * r, r)]
        return outs[k].at[at(owner * r, r), :]

    weights = []
    for k in range(3):
        for d, peer in enumerate((qa, qb, qd)):
            copy = remote(piece(k, peer), landing(k, f), w_s.at[k, d], w_r.at[k, d], fs=base + peer)
            copy.start()
            weights.append(copy)
    mine = at(c * half, half)
    near = []
    for i in range(3):
        for d, peer in enumerate((qa, qb)):
            copy = remote(xs[i].at[mine, :], ts[i].at[q, mine, :], n_s.at[i, d], n_r.at[i, d], fs=base + peer)
            copy.start()
            near.append(copy)
    local = []
    for k in range(3):
        copy = pltpu.make_async_copy(piece(k, q), landing(k, f), loc.at[k])
        copy.start()
        local.append(copy)
    for i in range(3):
        copy = pltpu.make_async_copy(xs[i], ts[i].at[q], loc.at[3 + i])
        copy.start()
        local.append(copy)

    def block(k, b):
        if k == 2:
            return od.at[:, at(b * GROUP * r, GROUP * r)]
        return outs[k].at[at(b * GROUP * r, GROUP * r), :]

    def right(k, s):
        b = block(k, z - s)
        return remote(b, b, r_s.at[s, k], r_r.at[s, k], fs=f + GROUP)

    def left(k, s):
        b = block(k, z + s)
        return remote(b, b, l_s.at[s, k], l_r.at[s, k], fs=f - GROUP)

    def arrived(k, s):
        @pl.when(z - s - 1 >= 0)
        def _():
            b = block(k, z - s - 1)
            remote(b, b, r_s.at[s, k], r_r.at[s, k], fs=f - GROUP).wait_recv()

        @pl.when(z + s + 1 < nz)
        def _():
            b = block(k, z + s + 1)
            remote(b, b, l_s.at[s, k], l_r.at[s, k], fs=f + GROUP).wait_recv()

    def onward(k, s, act):
        @pl.when(jnp.logical_and(z - s >= 0, last))
        def _():
            act(right(k, s))

        @pl.when(jnp.logical_and(z + s < nz, first))
        def _():
            act(left(k, s))

    begin, sent = (lambda copy: copy.start()), (lambda copy: copy.wait_send())

    row = lax.broadcasted_iota(jnp.int32, (rows, tile), 0)

    wide_tile = 2 * tile if d_model % (2 * tile) == 0 else tile

    def later(v, steps):
        return jnp.where(row >= steps, pltpu.roll(v, steps, 0), 0.0)

    def earlier(v, steps):
        return jnp.where(row < rows - steps, pltpu.roll(v, rows - steps, 0), 0.0)

    def forward(t, keep):
        @pl.loop(0, GROUP)
        def _(b):
            @pl.loop(0, u // tile)
            def _(j):
                cols, seq = at(j * tile, tile), at(b * rows, rows)
                x = t[b]
                gate = mm(x, og[:, cols]).astype(jnp.bfloat16).astype(jnp.float32)
                up = mm(x, ou[:, cols])
                conv = (bias[:, cols] + taps[2:3, cols] * gate + taps[1:2, cols] * later(gate, 1)
                        + taps[0:1, cols] * later(gate, 2))
                out = conv / (1.0 + jnp.exp(-conv)) * up
                if keep:
                    conv_s[seq, cols] = conv
                    up_s[seq, cols] = up
                    hid_t[at(j * tile, tile), seq] = out.T.astype(jnp.bfloat16)
                else:
                    hid[seq, cols] = out.astype(jnp.bfloat16)

    def down_grad():
        @pl.loop(0, d_model // wide_tile)
        def _(j):
            cols = at(j * wide_tile, wide_tile)
            cot = t2[:, :, cols].reshape(GROUP * rows, wide_tile)
            gp[:, cols] = mm(hid_t[...], cot).astype(jnp.bfloat16)

    def backward():
        @pl.loop(0, GROUP)
        def _(b):
            @pl.loop(0, u // tile)
            def _(j):
                cols, seq = at(j * tile, tile), at(b * rows, rows)
                dh = mm(t2[b], od[at(j * tile, tile), :], ((1,), (1,)))
                conv = conv_s[seq, cols]
                sig = 1.0 / (1.0 + jnp.exp(-conv))
                dup[seq, cols] = (dh * (conv * sig)).astype(jnp.bfloat16)
                dc = dh * up_s[seq, cols] * sig * (1.0 + conv * (1.0 - sig))
                dg = (taps[2:3, cols] * dc + taps[1:2, cols] * earlier(dc, 1)
                      + taps[0:1, cols] * earlier(dc, 2))
                dgate[seq, cols] = dg.astype(jnp.bfloat16)

    def late_out(owner):
        seq = at(owner * rows, rows)

        @pl.loop(0, d_model // wide_tile)
        def _(j):
            cols = at(j * wide_tile, wide_tile)
            yp[seq, cols] = mm(hid[seq, :], od[:, cols]).astype(jnp.bfloat16)

    def early_out(owner):
        seq = at(owner * rows, rows)

        @pl.loop(0, d_model // wide_tile)
        def _(j):
            cols = at(j * wide_tile, wide_tile)
            part = mm(dup[seq, :], ou[cols, :], ((1,), (1,))) + mm(dgate[seq, :], og[cols, :], ((1,), (1,)))
            xp[seq, cols] = part.astype(jnp.bfloat16)

    def enter(k):
        local[k].wait()
        for d in range(3):
            weights[3 * k + d].wait_recv()
        onward(k, 0, begin)

    enter(0)
    enter(1)
    partner = []

    def pass_on(i, owner, kind):
        there = ts[i].at[owner, mine, :]
        copy = remote(there, there, p_s.at[i, kind], p_r.at[i, kind], tp=1 - c)
        copy.start()
        partner.append((copy, i, owner, kind))

    far = []
    for i in range(3):
        near[2 * i].wait_recv()
        there = ts[i].at[qa, mine, :]
        copy = remote(there, there, n_s.at[i, 2], n_r.at[i, 2], fs=base + qb)
        copy.start()
        far.append(copy)
        pass_on(i, qa, 0)
        if i < 2 and nz > 2:
            arrived(i, 0)
            onward(i, 1, begin)
    for i in range(3):
        near[2 * i + 1].wait_recv()
        pass_on(i, qb, 1)
    for s in range(2, nz - 1):
        for k in range(2):
            arrived(k, s - 1)
            onward(k, s, begin)
    enter(2)
    for i in range(3):
        far[i].wait_recv()
        pass_on(i, qd, 2)
    if nz > 1:
        arrived(0, nz - 2)
        arrived(1, nz - 2)
    other = at((1 - c) * half, half)
    for copy, i, owner, kind in partner:
        there = ts[i].at[(qb, qa, qd)[kind], other, :]
        remote(there, there, p_s.at[i, kind], p_r.at[i, kind], tp=1 - c).wait_recv()
    for copy in local[3:]:
        copy.wait()

    jobs = [lambda: forward(t1, True), lambda: forward(t0, False), down_grad]
    for s in range(1, nz - 1):
        if jobs:
            jobs.pop(0)()
        arrived(2, s - 1)
        onward(2, s, begin)
    while jobs:
        jobs.pop(0)()
    grads = []
    for s in range(1, nz):
        to = lax.rem(z + s, nz)
        copy = remote(gp.at[:, at(to * wide, wide)], gin.at[s], z_s.at[s], z_r.at[s], fs=to * GROUP + q)
        copy.start()
        grads.append(copy)
    if nz > 1:
        arrived(2, nz - 2)

    parts, finals = (yp, xp), (y, dx)
    order = (qd, qa, qb, q)
    theirs = (qd, qb, qa, q)
    cores, sends = {}, {}

    def to_core(t, n):
        src = parts[t].at[at(theirs[n] * rows + (1 - c) * half, half), :]
        copy = remote(src, core.at[t, n], c_s.at[t, n], c_r.at[t, n], tp=1 - c)
        copy.start()
        cores[t, n] = copy

    def send(t, n, slot, peer):
        copy = remote(summed.at[t, n], got.at[t, slot], a_s.at[t, slot], a_r.at[t, slot], fs=base + peer)
        copy.start()
        sends[t, slot] = copy

    def join(t, n):
        cores[t, n].wait_recv()
        own = parts[t].at[at(order[n] * rows + c * half, half), :]
        total(summed.at[t, n], [own, core.at[t, n]], half)
        if n == 0:
            send(t, 0, 0, qa)
        if n == 1:
            send(t, 1, 1, qa)

    def onto_second(t):
        sends[t, 0].wait_recv()
        total(core.at[t, 0], [summed.at[t, 2], got.at[t, 0]], half)
        copy = remote(core.at[t, 0], got.at[t, 2], a_s.at[t, 2], a_r.at[t, 2], fs=base + qb)
        copy.start()
        sends[t, 2] = copy

    ends = []

    def finish(t):
        sends[t, 1].wait_recv()
        sends[t, 2].wait_recv()
        total(finals[t].at[mine, :], [summed.at[t, 3], got.at[t, 1], got.at[t, 2]], half)
        there = finals[t].at[mine, :]
        copy = remote(there, there, e_s.at[t], e_r.at[t], tp=1 - c)
        copy.start()
        ends.append(copy)

    def produce(t, make):
        make(qd)
        to_core(t, 0)
        make(qa)
        make(qb)
        to_core(t, 1)
        to_core(t, 2)
        join(t, 0)
        make(q)
        to_core(t, 3)
        for n in (1, 2):
            join(t, n)

    produce(0, late_out)
    backward()
    join(0, 3)
    onto_second(0)
    produce(1, early_out)
    join(1, 3)
    finish(0)
    onto_second(1)
    for copy in grads:
        copy.wait_recv()
    total(gsum, [gp.at[:, at(z * wide, wide)]] + [gin.at[s] for s in range(1, nz)], u)
    handed = []
    for d, peer in enumerate((qa, qb, qd)):
        copy = remote(gsum.at[:, at(peer * r, r)], g.at[at(q * u, u), :], g_s.at[d], g_r.at[d], fs=base + peer)
        copy.start()
        handed.append(copy)
    g[at(q * u, u), :] = gsum[:, at(q * r, r)]
    finish(1)
    for copy in handed + ends:
        copy.wait_recv()
    for copy in weights + near + far + [p[0] for p in partner]:
        copy.wait_send()
    for copy in list(cores.values()) + grads + handed + ends + list(sends.values()):
        copy.wait_send()
    for s in range(nz - 1):
        for k in range(3):
            onward(k, s, sent)


def layer(nz, xs, w_gate, w_up, w_down, taps, bias):
    rows, d = xs[0].shape
    u = w_gate.shape[1] // GROUP
    r = w_gate.shape[0]
    half, toks = rows // 2, GROUP * rows
    tile = 256 if u % 256 == 0 else 128
    sems = lambda *shape: [pltpu.SemaphoreType.DMA(shape)] * 2
    b16, f32 = jnp.bfloat16, jnp.float32
    out = jax.ShapeDtypeStruct((rows, d), b16)
    hops = max(nz - 1, 1)
    return pl.pallas_call(
        functools.partial(layer_kernel, nz, tile),
        out_shape=(out, out, jax.ShapeDtypeStruct((u * GROUP, r), b16)),
        in_specs=[VMEM] * 8,
        out_specs=(VMEM,) * 3,
        scratch_shapes=[pltpu.VMEM((GROUP, rows, d), b16)] * 3
        + [pltpu.VMEM((d, u), b16)] * 2
        + [pltpu.VMEM((u, d), b16), pltpu.VMEM((toks, u), b16), pltpu.VMEM((u, toks), b16),
           pltpu.VMEM((toks, u), f32), pltpu.VMEM((toks, u), f32),
           pltpu.VMEM((toks, u), b16), pltpu.VMEM((toks, u), b16),
           pltpu.VMEM((toks, d), b16), pltpu.VMEM((toks, d), b16), pltpu.VMEM((u, d), b16),
           pltpu.VMEM((2, 4, half, d), b16), pltpu.VMEM((2, 4, half, d), b16), pltpu.VMEM((2, 3, half, d), b16),
           pltpu.VMEM((nz, u, GROUP * r), b16), pltpu.VMEM((u, GROUP * r), b16),
           pltpu.SemaphoreType.DMA((6,))]
        + sems(3, 3) + sems(3, 3) + sems(3, 3) + sems(hops, 3) + sems(hops, 3)
        + sems(2, 4) + sems(2, 3) + sems(nz) + sems(3) + sems(2),
        compiler_params=pltpu.CompilerParams(collective_id=0, has_side_effects=True, vmem_limit_bytes=VMEM_BYTES),
        name="layer_group",
    )(*xs, w_gate, w_up, w_down, taps, bias)


def shift_later(field, steps):
    pad = jnp.zeros((steps, field.shape[1]), jnp.float32)
    return jnp.concatenate([pad, field[: field.shape[0] - steps]], axis=0)


def shift_earlier(field, steps):
    pad = jnp.zeros((steps, field.shape[1]), jnp.float32)
    return jnp.concatenate([field[steps:], pad], axis=0)


def contract_last(left, right):
    return lax.dot_general(
        left, right, (((1,), (1,)), ((), ())), preferred_element_type=jnp.float32
    )


def hidden_parts(inputs, gate_full, up_full, taps, bias):
    gate = (
        jnp.dot(inputs, gate_full, preferred_element_type=jnp.float32)
        .astype(jnp.bfloat16)
        .astype(jnp.float32)
    )
    up = jnp.dot(inputs, up_full, preferred_element_type=jnp.float32)
    conv = bias + taps[2] * gate + taps[1] * shift_later(gate, 1) + taps[0] * shift_later(gate, 2)
    act = jax.nn.silu(conv)
    hidden = (act * up).astype(jnp.bfloat16)
    return (conv, act, up, hidden)


def forward_pass(x_late, gate_full, up_full, down_full, taps, bias):
    conv, act, up, hidden = hidden_parts(x_late, gate_full, up_full, taps, bias)
    partial_value = jnp.dot(hidden, down_full, preferred_element_type=jnp.float32)
    return lax.psum(partial_value.astype(jnp.bfloat16), "tp")


def backward_pass(x_early, cotangent, gate_full, up_full, down_full, taps, bias, grad_down):
    conv, act, up, hidden = hidden_parts(x_early, gate_full, up_full, taps, bias)
    dhidden = contract_last(cotangent, down_full)
    summed = lax.psum_scatter(
        lax.dot_general(
            cotangent, hidden, (((0,), (0,)), ((), ())), preferred_element_type=jnp.float32
        ),
        "fs",
        scatter_dimension=0,
        tiled=True,
    )
    grad_down_out = grad_down + summed.T
    dup = (dhidden * act).astype(jnp.bfloat16)
    sig = jax.nn.sigmoid(conv)
    dconv = dhidden * up * sig * (1.0 + conv * (1.0 - sig))
    dgate = taps[2] * dconv + taps[1] * shift_earlier(dconv, 1) + taps[0] * shift_earlier(dconv, 2)
    dgate = dgate.astype(jnp.bfloat16)
    partial_value = contract_last(dup, up_full) + contract_last(dgate, gate_full)
    dx_early = lax.psum(partial_value.astype(jnp.bfloat16), "tp")
    return (dx_early, grad_down_out)


def shards(x_late, x_early, cotangent, w_gate, w_up, w_down, conv_taps, conv_bias, grad_down):
    width = w_gate.shape[1]
    offset = lax.axis_index("tp") * width
    taps = lax.dynamic_slice_in_dim(conv_taps, offset, width, 1)
    bias = lax.dynamic_slice_in_dim(conv_bias, offset, width, 0)
    gate_full, up_full = (
        lax.all_gather(w_gate, "fs", axis=0, tiled=True),
        lax.all_gather(w_up, "fs", axis=0, tiled=True),
    )
    down_full = lax.all_gather(w_down, "fs", axis=1, tiled=True)
    y_late = forward_pass(x_late, gate_full, up_full, down_full, taps, bias)
    dx_early, grad_down_out = backward_pass(
        x_early, cotangent, gate_full, up_full, down_full, taps, bias, grad_down
    )
    return (y_late, dx_early, grad_down_out)


def grouped_shards(nz, x_late, x_early, cotangent, w_gate, w_up, w_down, conv_taps, conv_bias, grad_down):
    units = w_gate.shape[1] // GROUP
    start = (lax.axis_index("tp") * GROUP + lax.rem(lax.axis_index("fs"), GROUP)) * units
    taps = lax.dynamic_slice_in_dim(conv_taps, start, units, 1)
    bias = lax.dynamic_slice_in_dim(conv_bias, start, units, 0)
    y_late, dx_early, grad = layer(
        nz, (x_late, x_early, cotangent), w_gate, w_up, w_down, taps, bias.reshape(1, units)
    )
    return (y_late, dx_early, grad_down + grad.astype(jnp.float32))


def solution(mesh):
    def step(*arrays):
        x_late, w_gate = arrays[0], arrays[3]
        fs, tp = mesh.shape["fs"], mesh.shape["tp"]
        units, rest = divmod(w_gate.shape[1], GROUP)
        lanes_ok = rest == 0 and units % 128 == 0 and w_gate.shape[0] % 128 == 0
        if tp == 2 and fs % GROUP == 0 and lanes_ok and x_late.shape[0] % 32 == 0:
            return grouped_shards(fs // GROUP, *arrays)
        return shards(*arrays)

    placed = (
        P("fs", None),
        P("fs", None),
        P("fs", None),
        P("fs", "tp"),
        P("fs", "tp"),
        P("tp", "fs"),
        P(),
        P(),
        P("tp", "fs"),
    )
    return jax.shard_map(
        step,
        mesh=mesh,
        in_specs=placed,
        out_specs=(P("fs", None), P("fs", None), P("tp", "fs")),
        check_vma=False,
    )
```
